32 devices in a mesh: ep: 16 (over z, y, core), tp: 2 (over x).
Axes of the slice: x: 2, y: 2, z: 4, core: 2. Of those that a mesh axis runs over, the one named last changes fastest.
Arguments:
- tokens: bfloat16 [256, 2048], P('ep'), may hold values from -6 to 6
- lengths: int32 [256], P('ep'), may hold values from 256 to 1023
- cache: bfloat16 [256, 1024, 512], P('ep', None, 'tp'), may hold values from -6 to 6
- attn_gain: float32 [2048], replicated, may hold values from 0.1 to 1.9
- query_weight: bfloat16 [2048, 1024], P(None, 'tp'), may hold values from -0.125 to 0.125
- key_weight: bfloat16 [2048, 256], P(None, 'tp'), may hold values from -0.125 to 0.125
- value_weight: bfloat16 [2048, 256], P(None, 'tp'), may hold values from -0.125 to 0.125
- stick_bias: float32 [16], P('tp'), may hold values from -7 to -1
- out_weight: bfloat16 [1024, 2048], P('tp'), may hold values from -0.1875 to 0.1875
- ffn_gain: float32 [2048], replicated, may hold values from 0.1 to 1.9
- routes: int32 [256, 6], P('ep'), may hold values from 0 to 15, all different within a row; in each aligned block of 16 rows (0 to 15, 16 to 31, ...) at most 12 rows name the same one
- route_weights: float32 [256, 6], P('ep'), may hold values from 0.1 to 0.6
- expert_gate: bfloat16 [16, 2048, 1024], P('ep', None, 'tp'), may hold values from -0.125 to 0.125
- expert_up: bfloat16 [16, 2048, 1024], P('ep', None, 'tp'), may hold values from -0.125 to 0.125
- expert_down: bfloat16 [16, 1024, 2048], P('ep', 'tp'), may hold values from -0.1875 to 0.1875
- shared_gate: bfloat16 [2048, 512], P('ep', 'tp'), may hold values from -0.125 to 0.125
- shared_up: bfloat16 [2048, 512], P('ep', 'tp'), may hold values from -0.125 to 0.125
- shared_down: bfloat16 [512, 2048], P('tp'), may hold values from -0.25 to 0.25
- gate_vector: bfloat16 [2048], replicated, may hold values from -0.125 to 0.125
Outputs:
- layer_out: bfloat16 [256, 2048], P('ep', 'tp')
- new_kv: bfloat16 [256, 512], P('ep', 'tp')
The draws below stay inside these ranges and needn't reach their ends.
Inputs may be any that keep to these rules, and one draw needn't show every extreme that they name: Each sequence's new token comes after its lengths cached positions. `routes`: each row names 6 different experts; among the 16 rows of one index of ep no expert is named by more than 12 rows.
All inputs are finite; a program needn't handle non-finite values.
Results may differ from the reference program's by a relative error of at most 0.012.
Values may be sent and summed in bfloat16 or wider, within the bound.
A program may use at most 64 MiB of HBM per device.

```python
import math
import jax
import jax.numpy as jnp
import numpy as np
from jax import lax

D = 2048
HEAD_DIM = 64
Q_HEADS = 16
KV_HEADS = 4
EXPERT_FF = 1024
SHARED_FF = 512
TOP_K = 6
SEQ_DEV = 16
CACHE = 1024
SEQS = 256
EXPERTS = 16
CAP = 12
N_EP = 16
N_TP = 2


def touch_ends(entries, own_key, low, largest):
    shape = entries.shape
    index_at = [jax.random.randint(jax.random.fold_in(own_key, axis), (), 0, shape[axis]) for axis in range(len(shape))]
    entries = entries.at[tuple(index_at)].set(low)
    longest = shape.index(max(shape))
    index_at[longest] = (index_at[longest] + 1) % shape[longest]
    return entries.at[tuple(index_at)].set(largest)


def steps_of(stream_key, dims, cuts, low, largest):
    def one(axis_at, parts):
        steps = jax.random.uniform(jax.random.fold_in(jax.random.fold_in(stream_key, 6), axis_at), (parts,), jnp.float32, low / len(cuts), largest / len(cuts))
        return jnp.repeat(jnp.exp(steps), dims[axis_at] // parts).reshape((-1,) + (1,) * (len(dims) - axis_at - 1))

    factor_of = one(*cuts[0])
    for cut in cuts[1:]:
        factor_of = factor_of * one(*cut)
    return factor_of


def routed_block(rng, own, number, rows, count, top, bound, lean):
    sequence = jax.random.permutation(rng, count)
    heavy_load, usual = shares(count, rows * top, bound, lean, True), shares(count, rows * top, bound, lean, False)
    places = jnp.arange(count)

    def named(tallies, turn):
        used = int((tallies > 0).sum())
        fixed = max(1, used // 4)
        passed = fixed + (places - fixed + turn * (used - fixed)) % max(1, count - fixed)
        return jnp.zeros((count,), jnp.int32).at[sequence[jnp.where(places < fixed, places, passed)]].set(jnp.asarray(tallies, jnp.int32))

    tallies = jnp.where(number % 4 == 0, named(heavy_load, number // 4), named(usual, number - number // 4 - 1))
    mixed = jax.random.permutation(jax.random.fold_in(own, 3), count)
    source_of, sink = mixed[0:count // 2 * 2:2], mixed[1:count // 2 * 2:2]
    slack = jnp.minimum(tallies[source_of] - 1, bound - tallies[sink]) // 2
    slack = jnp.where((source_of == sequence[0]) | (sink == sequence[0]) | (tallies[sink] == 0), 0, jnp.maximum(slack, 0))
    passed = jax.random.randint(jax.random.fold_in(own, 4), (count // 2,), 0, 1 << 20) % (slack + 1)
    tallies = tallies.at[source_of].add(-passed).at[sink].add(passed)
    items = jnp.searchsorted(jnp.cumsum(tallies), jnp.arange(rows * top), side="right").astype(jnp.int32)
    table = items.reshape(top, rows).T
    table = table[jax.random.permutation(jax.random.fold_in(own, 1), rows)]
    turn = jax.random.randint(jax.random.fold_in(own, 2), (rows, 1), 0, top)
    return jnp.take_along_axis(table, (jnp.arange(top)[None, :] + turn) % top, axis=1)


def shares(count, total, most, skew, full):
    loads = [(1 << 20) // math.isqrt(standing ** skew) + 1 for standing in range(1, count + 1)]
    largest = most if full else min(most, max(-(-total // count), total * loads[0] // sum(loads)))
    least = 1 if total - largest >= count - 1 else 0
    given, surplus = [largest] + [least] * (count - 1), total - largest - least * (count - 1)
    while surplus > 0:
        free = [i for i in range(1, count) if given[i] < largest] or [i for i in range(1, count) if given[i] < most]
        pool, remaining = sum([loads[i] for i in free]), surplus
        for i in free:
            addition = min(most - given[i], max(1, remaining * loads[i] // pool), surplus)
            given[i] = given[i] + addition
            surplus = surplus - addition
    return np.array(given)


def noise(rng, shape, spread, most, shards=(), kind=jnp.bfloat16):
    values = jax.random.normal(rng, shape, jnp.float32) * spread
    if len(shards) > 0:
        values = steps_of(rng, shape, shards, -0.22, 0.18) * values
    return jnp.clip(values, min=-most, max=most).astype(kind)


def setup_inputs(seed: int = 0) -> dict:
    splits = jax.random.split(jax.random.key(seed), 20)
    tokens = noise(splits[0], (SEQS, D), 1.0, 6.0, ((0, 16),))
    lengths = touch_ends(jax.random.randint(splits[1], (SEQS,), CACHE // 4, CACHE), jax.random.fold_in(splits[1], 1), CACHE // 4, CACHE - 1).astype(jnp.int32)
    cache = noise(splits[2], (SEQS, CACHE, 2 * KV_HEADS * HEAD_DIM), 1.0, 6.0, ((0, 16), (2, 2)))
    attn_gain = jnp.clip(1.0 + 0.18 * jax.random.normal(splits[3], (D,), jnp.float32), 0.1, 1.9)
    query_weight = noise(splits[4], (D, Q_HEADS * HEAD_DIM), D ** -0.5, 0.125, ((1, 2),))
    key_weight = noise(splits[5], (D, KV_HEADS * HEAD_DIM), D ** -0.5, 0.125, ((1, 2),))
    value_weight = noise(splits[6], (D, KV_HEADS * HEAD_DIM), D ** -0.5, 0.125, ((1, 2),))
    stick_bias = jnp.clip(-7.0 + 6.0 * jax.random.uniform(splits[7], (Q_HEADS,), jnp.float32) ** steps_of(splits[7], (Q_HEADS,), ((0, 2),), -0.2, 0.2), -7.0, -1.0)
    out_weight = noise(splits[8], (Q_HEADS * HEAD_DIM, D), (Q_HEADS * HEAD_DIM) ** -0.5, 0.1875, ((0, 2),))
    ffn_gain = jnp.clip(1.0 + 0.18 * jax.random.normal(splits[9], (D,), jnp.float32), 0.1, 1.9)
    routes_keys = jax.random.split(jax.random.fold_in(splits[10], 1), SEQS // SEQ_DEV)
    routes_turns = jax.random.permutation(jax.random.fold_in(splits[10], 3), SEQS // SEQ_DEV)
    routes = jax.vmap(lambda own, number: routed_block(jax.random.fold_in(splits[10], 2), own, number, SEQ_DEV, EXPERTS, TOP_K, CAP, 1))(routes_keys, routes_turns).reshape((SEQS, TOP_K))
    route_weights = jnp.clip(0.1 + 0.5 * jax.random.uniform(splits[11], (SEQS, TOP_K), jnp.float32) ** steps_of(splits[11], (SEQS, TOP_K), ((0, 16),), -0.2, 0.2), 0.1, 0.6)
    expert_gate = noise(splits[12], (EXPERTS, D, EXPERT_FF), D ** -0.5, 0.125, ((0, 16), (2, 2)))
    expert_up = noise(splits[13], (EXPERTS, D, EXPERT_FF), D ** -0.5, 0.125, ((0, 16), (2, 2)))
    expert_down = noise(splits[14], (EXPERTS, EXPERT_FF, D), EXPERT_FF ** -0.5, 0.1875, ((0, 16), (1, 2)))
    shared_gate = noise(splits[15], (D, SHARED_FF), D ** -0.5, 0.125, ((0, 16), (1, 2)))
    shared_up = noise(splits[16], (D, SHARED_FF), D ** -0.5, 0.125, ((0, 16), (1, 2)))
    shared_down = noise(splits[17], (SHARED_FF, D), SHARED_FF ** -0.5, 0.25, ((0, 2),))
    gate_vector = noise(splits[18], (D,), D ** -0.5, 0.125)
    return dict(tokens=tokens, lengths=lengths, cache=cache, attn_gain=attn_gain, query_weight=query_weight, key_weight=key_weight, value_weight=value_weight, stick_bias=stick_bias, out_weight=out_weight, ffn_gain=ffn_gain, routes=routes, route_weights=route_weights, expert_gate=expert_gate, expert_up=expert_up, expert_down=expert_down, shared_gate=shared_gate, shared_up=shared_up, shared_down=shared_down, gate_vector=gate_vector)


epsilon = 1e-06

def rms_scale(rows_in, gain_row):
    values_f = rows_in.astype(jnp.float32)
    return values_f * lax.rsqrt(lax.optimization_barrier(jnp.mean(values_f * values_f, axis=-1, keepdims=True)) + epsilon) * gain_row

def block_sum(left_rows, right_rows, blocks):
    row_count, inner = left_rows.shape
    part_width = inner // blocks
    left_view = left_rows.reshape(row_count, blocks, part_width).astype(jnp.float32)
    right_view = right_rows.reshape(blocks, part_width, right_rows.shape[1]).astype(jnp.float32)
    partials = jnp.einsum('nbf,bfd->bnd', left_view, right_view).astype(jnp.bfloat16)
    return lax.optimization_barrier(jnp.sum(partials.astype(jnp.float32), axis=0))

def reference(tokens, lengths, cache, attn_gain, query_weight, key_weight, value_weight, stick_bias, out_weight, ffn_gain, routes, route_weights, expert_gate, expert_up, expert_down, shared_gate, shared_up, shared_down, gate_vector):
    total_rows = tokens.shape[0]
    normed = rms_scale(tokens, attn_gain).astype(jnp.bfloat16)
    queries = jnp.dot(normed, query_weight, preferred_element_type=jnp.float32).astype(jnp.bfloat16)
    key_rows = jnp.dot(normed, key_weight, preferred_element_type=jnp.float32).astype(jnp.bfloat16)
    value_rows = jnp.dot(normed, value_weight, preferred_element_type=jnp.float32).astype(jnp.bfloat16)
    new_kv = jnp.stack([key_rows.reshape(total_rows, KV_HEADS, HEAD_DIM), value_rows.reshape(total_rows, KV_HEADS, HEAD_DIM)], axis=2)
    new_kv = new_kv.reshape(total_rows, 2 * KV_HEADS * HEAD_DIM)
    group_size = Q_HEADS // KV_HEADS
    grouped = queries.reshape(N_EP, SEQ_DEV, KV_HEADS, group_size, HEAD_DIM)
    cache_view = cache.reshape(N_EP, SEQ_DEV, CACHE, KV_HEADS, 2, HEAD_DIM)
    span_rows = lengths.reshape(N_EP, SEQ_DEV)
    offsets = stick_bias.astype(jnp.float32).reshape(1, KV_HEADS, group_size, 1)

    def attend(pieces):
        query_block, cache_block, span_block = pieces
        key_block = cache_block[:, :, :, 0, :].astype(jnp.float32)
        value_block = cache_block[:, :, :, 1, :].astype(jnp.float32)
        scores = jnp.einsum('nkgd,nckd->nkgc', query_block.astype(jnp.float32), key_block) * HEAD_DIM ** (-0.5)
        scores = scores + offsets
        positions = jnp.arange(CACHE, dtype=jnp.int32)
        usable = (positions[None, :] < span_block[:, None])[:, None, None, :]
        log_keep = jnp.where(usable, jax.nn.log_sigmoid(-scores), 0.0)
        behind = lax.cumsum(log_keep, axis=3, reverse=True) - log_keep
        stick_weights = jnp.where(usable, jnp.exp(jax.nn.log_sigmoid(scores) + behind), 0.0).astype(jnp.bfloat16)
        mixed = jnp.einsum('nkgc,nckd->nkgd', stick_weights.astype(jnp.float32), value_block)
        return mixed.astype(jnp.bfloat16)
    heads_out = lax.map(attend, (grouped, cache_view, span_rows)).reshape(total_rows, Q_HEADS * HEAD_DIM)
    residual = tokens.astype(jnp.float32) + block_sum(heads_out, out_weight, N_TP)
    normed_mix = rms_scale(residual, ffn_gain).astype(jnp.bfloat16)
    flat_routes = routes.reshape(-1)
    flat_weights = route_weights.reshape(-1).astype(jnp.float32)
    rows_most = N_EP * CAP

    def run_expert(expert_index):
        routed_here = flat_routes == expert_index
        ordering = jnp.argsort(jnp.where(routed_here, 0, 1).astype(jnp.int32), stable=True)[:rows_most]
        ordering = ordering.astype(jnp.int32)
        owners = (ordering // TOP_K).astype(jnp.int32)
        chosen = normed_mix[owners]
        gate_val = jnp.dot(chosen, expert_gate[expert_index], preferred_element_type=jnp.float32)
        up_val = jnp.dot(chosen, expert_up[expert_index], preferred_element_type=jnp.float32)
        hidden = (jax.nn.silu(gate_val) * up_val).astype(jnp.bfloat16)
        result = block_sum(hidden, expert_down[expert_index], N_TP).astype(jnp.bfloat16)
        route_scale = jnp.where(routed_here[ordering], flat_weights[ordering], 0.0)
        return (owners, result.astype(jnp.float32) * route_scale[:, None])
    owner_rows, contrib = lax.map(run_expert, jnp.arange(EXPERTS, dtype=jnp.int32))
    routed = jnp.zeros((total_rows, D), jnp.float32).at[owner_rows.reshape(-1)].add(contrib.reshape(-1, D))
    shared_gate_val = jnp.dot(normed_mix, shared_gate, preferred_element_type=jnp.float32)
    shared_up_val = jnp.dot(normed_mix, shared_up, preferred_element_type=jnp.float32)
    shared_hidden = (jax.nn.silu(shared_gate_val) * shared_up_val).astype(jnp.bfloat16)
    shared_out = block_sum(shared_hidden, shared_down, N_TP)
    mix_gate = jax.nn.sigmoid(jnp.dot(normed_mix, gate_vector, preferred_element_type=jnp.float32))
    layer_out = (residual + routed + mix_gate[:, None] * shared_out).astype(jnp.bfloat16)
    return (layer_out, new_kv)
```

```python
import functools

import jax
import jax.numpy as jnp
from jax import lax
from jax.experimental import pallas as pl
from jax.experimental.pallas import tpu as pltpu
from jax.sharding import PartitionSpec as P

HEAD_DIM = 64
LANES = 128
epsilon = 1e-06
MESH = pl.DeviceIdType.MESH
F32 = jnp.float32
BF16 = jnp.bfloat16


def rms_scale(rows_in, gain_row):
    values_f = rows_in.astype(F32)
    return (
        values_f
        * lax.rsqrt(jnp.mean(values_f * values_f, axis=-1, keepdims=True) + epsilon)
        * gain_row
    )


def attend_kernel(groups, query_ref, span_ref, bias_ref, cache_ref, out_ref, held, logits, sems):
    seqs, heads, _ = query_ref.shape
    length = cache_ref.shape[1]
    width = 256
    count = length // width
    copies = []
    for s in range(seqs):
        copy = pltpu.make_async_copy(cache_ref.at[s], held.at[s], sems.at[s])
        copy.start()
        copies.append(copy)
    table = (
        lax.broadcasted_iota(jnp.int32, (width, width), 0)
        >= lax.broadcasted_iota(jnp.int32, (width, width), 1)
    ).astype(F32)
    per_group = seqs // groups
    rows = per_group * heads
    for g in range(groups):
        first = g * per_group
        for s in range(first, first + per_group):
            copies[s].wait()
            logits[s * heads : (s + 1) * heads, :] = lax.dot_general(
                query_ref[s], held[s], (((1,), (1,)), ((), ())), preferred_element_type=F32
            )
        span = slice(first * heads, first * heads + rows)
        limit = span_ref[span, :]
        offset = bias_ref[span, :]
        carried = jnp.zeros((rows, 1), F32)
        for b in range(count - 1, -1, -1):
            cols = slice(b * width, (b + 1) * width)
            z = logits[span, cols] * HEAD_DIM ** (-0.5) + offset
            position = lax.broadcasted_iota(jnp.int32, (rows, width), 1) + b * width
            usable = position < limit
            soft = jnp.where(usable, jnp.maximum(z, 0.0) + jnp.log1p(jnp.exp(-jnp.abs(z))), 0.0)
            behind = jnp.dot(soft, table, precision=lax.Precision.HIGHEST, preferred_element_type=F32)
            weight = jnp.where(usable, jnp.exp(z - behind - carried), 0.0)
            carried = carried + jnp.sum(soft, axis=1, keepdims=True)
            logits[span, cols] = weight
        for s in range(first, first + per_group):
            out_ref[s] = jnp.dot(
                logits[s * heads : (s + 1) * heads, :].astype(BF16),
                held[s],
                preferred_element_type=F32,
            )


def attend(query_grid, lengths, bias, cache):
    seqs, heads, lanes = query_grid.shape
    length = cache.shape[1]
    span_rows = jnp.repeat(lengths, heads).reshape(seqs * heads, 1)
    bias_rows = jnp.tile(bias, seqs).reshape(seqs * heads, 1)
    vmem = pl.BlockSpec(memory_space=pltpu.VMEM)
    return pl.pallas_call(
        functools.partial(attend_kernel, 2),
        out_shape=jax.ShapeDtypeStruct((seqs, heads, lanes), F32),
        in_specs=[vmem, vmem, vmem, pl.BlockSpec(memory_space=pl.ANY)],
        out_specs=vmem,
        scratch_shapes=[
            pltpu.VMEM((seqs, length, lanes), BF16),
            pltpu.VMEM((seqs * heads, length), F32),
            pltpu.SemaphoreType.DMA((seqs,)),
        ],
        compiler_params=pltpu.CompilerParams(vmem_limit_bytes=60 * 2**20),
    )(query_grid, span_rows, bias_rows, cache)


def mix_kernel(
    ranks_ep,
    ranks_tp,
    partial_ref,
    tokens_ref,
    gain_ref,
    vector_ref,
    route_ref,
    sgate_ref,
    sup_ref,
    sdown_hbm,
    gate_hbm,
    up_hbm,
    down_hbm,
    out_ref,
    attn_in,
    residual_ref,
    gathered,
    hidden_ref,
    terms,
    terms_in,
    shared,
    shared_in,
    last,
    last_in,
    gate_w,
    up_w,
    down_w,
    sdown_w,
    load_sem,
    tp_send,
    tp_recv,
    ag_send,
    ag_recv,
    rs_send,
    rs_recv,
    sh_send,
    sh_recv,
    out_send,
    out_recv,
):
    me = lax.axis_index("ep")
    my_tp = lax.axis_index("tp")
    row_count, width = tokens_ref.shape
    experts = gate_w.shape[0]
    bits = ranks_ep.bit_length() - 1
    weights = [ranks_ep >> (i + 1) for i in range(bits)]
    mine = [(me // w) % 2 for w in weights]
    partner = [me + (1 - 2 * mine[i]) * weights[i] for i in range(bits)]
    all_rows = ranks_ep * row_count

    loads = []
    for i, (source, target) in enumerate(
        ((gate_hbm, gate_w), (up_hbm, up_w), (down_hbm, down_w), (sdown_hbm, sdown_w))
    ):
        load = pltpu.make_async_copy(source, target, load_sem.at[i])
        load.start()
        loads.append(load)

    barrier = pltpu.get_barrier_semaphore()
    for i in range(bits):
        pl.semaphore_signal(barrier, inc=1, device_id={"ep": partner[i]}, device_id_type=MESH)
    for step in range(1, ranks_tp):
        pl.semaphore_signal(
            barrier, inc=1, device_id={"tp": lax.rem(my_tp + step, ranks_tp)}, device_id_type=MESH
        )
    pl.semaphore_wait(barrier, bits + ranks_tp - 1)

    swaps = []
    for step in range(1, ranks_tp):
        swap = pltpu.make_async_remote_copy(
            src_ref=partial_ref,
            dst_ref=attn_in.at[step - 1],
            send_sem=tp_send.at[step - 1],
            recv_sem=tp_recv.at[step - 1],
            device_id={"tp": lax.rem(my_tp + step, ranks_tp)},
            device_id_type=MESH,
        )
        swap.start()
        swaps.append(swap)
    residual = partial_ref[...].astype(F32)
    for step in range(1, ranks_tp):
        swaps[step - 1].wait()
        residual = residual + attn_in[step - 1].astype(F32)
    residual = residual + tokens_ref[...].astype(F32)
    residual_ref[...] = residual
    normed = (
        residual
        * lax.rsqrt(jnp.mean(residual * residual, axis=-1, keepdims=True) + epsilon)
        * gain_ref[...]
    ).astype(BF16)
    gathered[(*mine, slice(None), pl.ds(0, width))] = normed
    gathered[(*mine, slice(None), pl.ds(width, route_ref.shape[1]))] = route_ref[...]
    mix_gate = jax.nn.sigmoid(
        jnp.sum(normed.astype(F32) * vector_ref[...].astype(F32), axis=1, keepdims=True)
    )

    core = bits - 1
    near = max(bits - 2, 0)
    others = [i for i in range(bits) if i not in (core, near)]
    orders = ([*others, near, core], [near, *others, core])
    orders = tuple(list(dict.fromkeys(order)) for order in orders)
    half = width // 2
    spans = (pl.ds(0, half), pl.ds(half, gathered.shape[-1] - half))

    def region(done):
        return tuple(slice(None) if i in done else mine[i] for i in range(bits))

    pulls = {}
    for turn in range(bits):
        for s in range(2):
            if turn > 0:
                pulls[s, turn - 1].wait_recv()
            axis = orders[s][turn]
            where = (*region(orders[s][:turn]), slice(None), spans[s])
            pull = pltpu.make_async_remote_copy(
                src_ref=gathered.at[where],
                dst_ref=gathered.at[where],
                send_sem=ag_send.at[s, turn],
                recv_sem=ag_recv.at[s, turn],
                device_id={"ep": partner[axis]},
                device_id_type=MESH,
            )
            pull.start()
            pulls[s, turn] = pull
    for s in range(2):
        pulls[s, bits - 1].wait_recv()
    for pull in pulls.values():
        pull.wait_send()

    def reduce_at(fixed, axis, other):
        return tuple(
            (1 - mine[i] if other else mine[i]) if i == axis else mine[i] if i in fixed else slice(None)
            for i in range(bits)
        )

    def push(source, landing, order, turn, cols, send, recv):
        axis = order[turn]
        copy = pltpu.make_async_remote_copy(
            src_ref=source.at[(*reduce_at(order[:turn], axis, True), slice(None), cols)],
            dst_ref=landing.at[(*reduce_at(order[:turn], axis, False), slice(None), cols)],
            send_sem=send,
            recv_sem=recv,
            device_id={"ep": partner[axis]},
            device_id_type=MESH,
        )
        copy.start()
        return copy

    def fold(source, landing, order, turn, cols):
        axis = order[turn]
        own = (*reduce_at(order[:turn], axis, False), slice(None), cols)
        came = (*reduce_at(order[:turn], axis, True), slice(None), cols)
        return source[own].astype(F32) + landing[came].astype(F32), own

    shared_cols = sgate_ref.shape[1]
    depth = sgate_ref.shape[0]
    feature_at = pl.ds(pl.multiple_of(me * (width // ranks_ep) // depth * depth, depth), depth)
    everyone = (slice(None),) * bits
    features = gathered[(*everyone, slice(None), feature_at)].reshape(all_rows, depth)
    grid = tuple(2 for _ in range(bits)) + (row_count,)
    for i, part in enumerate((sgate_ref, sup_ref)):
        shared[(*everyone, slice(None), pl.ds(i * shared_cols, shared_cols))] = (
            jnp.dot(features, part[...], preferred_element_type=F32)
            .astype(BF16)
            .reshape(*grid, shared_cols)
        )
    shared_order = orders[0][::-1]
    shared_span = pl.ds(0, 2 * shared_cols)
    state = {"turn": -1, "copies": []}

    def advance_shared():
        turn = state["turn"]
        total = None
        if turn >= 0:
            state["copies"][turn].wait_recv()
            total, own = fold(shared, shared_in, shared_order, turn, shared_span)
            if turn < bits - 1:
                shared[own] = total.astype(BF16)
        if turn < bits - 1:
            turn = turn + 1
            state["turn"] = turn
            state["copies"].append(
                push(
                    shared,
                    shared_in,
                    shared_order,
                    turn,
                    shared_span,
                    sh_send.at[turn],
                    sh_recv.at[turn],
                )
            )
        return total

    advance_shared()
    rows = gathered[(*everyone, slice(None), pl.ds(0, width))].reshape(all_rows, width)
    route_cols = gathered[
        (*everyone, slice(None), pl.ds(width, route_ref.shape[1]))
    ].reshape(all_rows, route_ref.shape[1])
    lane = lax.broadcasted_iota(jnp.int32, route_cols.shape, 1)
    stride = route_ref.shape[1] // 2
    route_cols = route_cols.astype(F32)
    loads[0].wait()
    loads[1].wait()
    scales = []
    for j in range(experts):
        wanted = me * experts + j
        chosen = jnp.where((lane == wanted) | (lane == wanted + stride), route_cols, 0.0)
        scales.append(jnp.sum(chosen, axis=1, keepdims=True))
        gate_val = jnp.dot(rows, gate_w[j], preferred_element_type=F32)
        up_val = jnp.dot(rows, up_w[j], preferred_element_type=F32)
        hidden_ref[j] = (gate_val * jax.nn.sigmoid(gate_val) * up_val).astype(BF16)
    total = advance_shared()
    loads[2].wait()
    loads[3].wait()
    reduce_orders = tuple(order[::-1] for order in ([*orders[0]], [*orders[1]]))
    reduce_spans = (pl.ds(0, half), pl.ds(half, width - half))
    sums = {}
    for s in range(2):
        term = jnp.zeros((all_rows, half), F32)
        for j in range(experts):
            term = term + scales[j] * jnp.dot(
                hidden_ref[j], down_w[j, :, s * half : (s + 1) * half], preferred_element_type=F32
            )
        terms[(*everyone, slice(None), reduce_spans[s])] = term.astype(BF16).reshape(*grid, half)
        sums[s, 0] = push(
            terms, terms_in, reduce_orders[s], 0, reduce_spans[s], rs_send.at[s, 0], rs_recv.at[s, 0]
        )
        total = advance_shared() if state["turn"] < bits - 1 else total
    pieces = []
    for turn in range(bits):
        for s in range(2):
            sums[s, turn].wait_recv()
            value, own = fold(terms, terms_in, reduce_orders[s], turn, reduce_spans[s])
            if turn < bits - 1:
                terms[own] = value.astype(BF16)
                sums[s, turn + 1] = push(
                    terms,
                    terms_in,
                    reduce_orders[s],
                    turn + 1,
                    reduce_spans[s],
                    rs_send.at[s, turn + 1],
                    rs_recv.at[s, turn + 1],
                )
            else:
                pieces.append(value)
        if turn == 0:
            while state["turn"] < bits - 1:
                advance_shared()
            total = advance_shared()
            gate_sum = total[:, :shared_cols]
            up_sum = total[:, shared_cols:]
            shared_hidden = (gate_sum * jax.nn.sigmoid(gate_sum) * up_sum).astype(BF16)
            shared_term = mix_gate * jnp.dot(
                shared_hidden, sdown_w[...], preferred_element_type=F32
            )
    for copy in (*sums.values(), *state["copies"]):
        copy.wait_send()
    for s in range(2):
        cols = slice(s * half, (s + 1) * half)
        last[:, cols] = (pieces[s] + shared_term[:, cols]).astype(BF16)
    quarter = width // ranks_tp

    def quarter_of(index):
        return pl.ds(pl.multiple_of(index * quarter, quarter), quarter)

    ends = []
    for step in range(1, ranks_tp):
        goal = lax.rem(my_tp + step, ranks_tp)
        end = pltpu.make_async_remote_copy(
            src_ref=last.at[:, quarter_of(goal)],
            dst_ref=last_in.at[step - 1],
            send_sem=out_send.at[step - 1],
            recv_sem=out_recv.at[step - 1],
            device_id={"tp": goal},
            device_id_type=MESH,
        )
        end.start()
        ends.append(end)
    result = residual_ref[:, quarter_of(my_tp)] + last[:, quarter_of(my_tp)].astype(F32)
    for step in range(1, ranks_tp):
        ends[step - 1].wait()
        result = result + last_in[step - 1].astype(F32)
    out_ref[...] = result.astype(BF16)


def mix(
    ranks_ep,
    ranks_tp,
    attn_term,
    tokens,
    ffn_gain,
    gate_vector,
    route_table,
    shared_gate,
    shared_up,
    shared_down,
    expert_gate,
    expert_up,
    expert_down,
):
    row_count, width = tokens.shape
    bits = ranks_ep.bit_length() - 1
    grid = (2,) * bits + (row_count,)
    experts, _, hidden = expert_gate.shape
    shared_cols = shared_gate.shape[1]
    quarter = width // ranks_tp
    swaps = max(ranks_tp - 1, 1)
    vmem = pl.BlockSpec(memory_space=pltpu.VMEM)
    anywhere = pl.BlockSpec(memory_space=pl.ANY)
    dma = pltpu.SemaphoreType.DMA
    return pl.pallas_call(
        functools.partial(mix_kernel, ranks_ep, ranks_tp),
        out_shape=jax.ShapeDtypeStruct((row_count, quarter), BF16),
        in_specs=[vmem] * 7 + [anywhere] * 4,
        out_specs=vmem,
        scratch_shapes=[
            pltpu.VMEM((swaps, row_count, width), BF16),
            pltpu.VMEM((row_count, width), F32),
            pltpu.VMEM((*grid, width + route_table.shape[1]), BF16),
            pltpu.VMEM((experts, ranks_ep * row_count, hidden), BF16),
            pltpu.VMEM((*grid, width), BF16),
            pltpu.VMEM((*grid, width), BF16),
            pltpu.VMEM((*grid, 2 * shared_cols), BF16),
            pltpu.VMEM((*grid, 2 * shared_cols), BF16),
            pltpu.VMEM((row_count, width), BF16),
            pltpu.VMEM((swaps, row_count, quarter), BF16),
            pltpu.VMEM(expert_gate.shape, BF16),
            pltpu.VMEM(expert_up.shape, BF16),
            pltpu.VMEM(expert_down.shape, BF16),
            pltpu.VMEM(shared_down.shape, BF16),
            dma((4,)),
            dma((swaps,)),
            dma((swaps,)),
            dma((2, bits)),
            dma((2, bits)),
            dma((2, bits)),
            dma((2, bits)),
            dma((bits,)),
            dma((bits,)),
            dma((swaps,)),
            dma((swaps,)),
        ],
        compiler_params=pltpu.CompilerParams(
            collective_id=0, has_side_effects=True, vmem_limit_bytes=60 * 2**20
        ),
    )(
        attn_term,
        tokens,
        ffn_gain.reshape(1, width),
        gate_vector.reshape(1, width),
        route_table,
        shared_gate,
        shared_up,
        shared_down,
        expert_gate,
        expert_up,
        expert_down,
    )


def shards(
    ranks_ep,
    ranks_tp,
    tokens,
    lengths,
    cache,
    attn_gain,
    query_weight,
    key_weight,
    value_weight,
    stick_bias,
    out_weight,
    ffn_gain,
    routes,
    route_weights,
    expert_gate,
    expert_up,
    expert_down,
    shared_gate,
    shared_up,
    shared_down,
    gate_vector,
):
    row_count = tokens.shape[0]
    normed = rms_scale(tokens, attn_gain).astype(BF16)
    queries = jnp.dot(normed, query_weight, preferred_element_type=F32).astype(BF16)
    key_rows = jnp.dot(normed, key_weight, preferred_element_type=F32).astype(BF16)
    value_rows = jnp.dot(normed, value_weight, preferred_element_type=F32).astype(BF16)
    heads = key_weight.shape[1] // HEAD_DIM
    new_kv = jnp.stack(
        [
            key_rows.reshape(row_count, heads, HEAD_DIM),
            value_rows.reshape(row_count, heads, HEAD_DIM),
        ],
        axis=2,
    ).reshape(row_count, heads * 2 * HEAD_DIM)
    group = queries.shape[1] // HEAD_DIM // heads
    same = jnp.eye(heads, dtype=jnp.bool_)
    spread = jnp.where(
        same[None, :, None, :, None],
        queries.reshape(row_count, heads, group, 1, HEAD_DIM),
        jnp.zeros((), BF16),
    )
    spread = jnp.pad(spread, ((0, 0),) * 4 + ((0, HEAD_DIM),))
    query_grid = spread.reshape(row_count, heads * group, heads * 2 * HEAD_DIM)
    mixed = attend(query_grid, lengths, stick_bias, cache)
    mixed = mixed.reshape(row_count, heads, group, heads, 2 * HEAD_DIM)[..., HEAD_DIM:]
    heads_out = jnp.sum(jnp.where(same[None, :, None, :, None], mixed, 0.0), axis=3).astype(BF16)
    attn_term = jnp.dot(
        heads_out.reshape(row_count, -1), out_weight, preferred_element_type=F32
    ).astype(BF16)
    experts_all = ranks_ep * expert_gate.shape[0]
    stride = -(-2 * experts_all // LANES) * LANES // 2
    named = routes[:, :, None] == lax.broadcasted_iota(jnp.int32, (1, 1, stride), 2)
    dense = jnp.sum(jnp.where(named, route_weights[:, :, None], 0.0), axis=1)
    high = lax.reduce_precision(dense, 8, 7)
    route_table = jnp.concatenate([high, dense - high], axis=1).astype(BF16)
    depth = shared_gate.shape[0]
    if depth % LANES:
        slot = lax.axis_index("ep") * depth % LANES
        wide = jnp.zeros((LANES, shared_gate.shape[1]), BF16)
        shared_gate = lax.dynamic_update_slice_in_dim(wide, shared_gate, slot, 0)
        shared_up = lax.dynamic_update_slice_in_dim(wide, shared_up, slot, 0)
    layer_out = mix(
        ranks_ep,
        ranks_tp,
        attn_term,
        tokens,
        ffn_gain,
        gate_vector,
        route_table,
        shared_gate,
        shared_up,
        shared_down,
        expert_gate,
        expert_up,
        expert_down,
    )
    return (layer_out, new_kv)


def solution(mesh):
    placed = (
        P("ep", None),
        P("ep"),
        P("ep", None, "tp"),
        P(),
        P(None, "tp"),
        P(None, "tp"),
        P(None, "tp"),
        P("tp"),
        P("tp", None),
        P(),
        P("ep", None),
        P("ep", None),
        P("ep", None, "tp"),
        P("ep", None, "tp"),
        P("ep", "tp", None),
        P("ep", "tp"),
        P("ep", "tp"),
        P("tp", None),
        P(),
    )
    return jax.shard_map(
        functools.partial(shards, mesh.shape["ep"], mesh.shape["tp"]),
        mesh=mesh,
        in_specs=placed,
        out_specs=(P("ep", "tp"), P("ep", "tp")),
        check_vma=False,
    )
```

```python
import functools

import jax
import jax.numpy as jnp
from jax import lax
from jax.experimental import pallas as pl
from jax.experimental.pallas import tpu as pltpu
from jax.sharding import PartitionSpec as P

HEAD_DIM = 64
LANES = 128
epsilon = 1e-06
MESH = pl.DeviceIdType.MESH
F32 = jnp.float32
BF16 = jnp.bfloat16


def rms_scale(rows_in, gain_row):
    values_f = rows_in.astype(F32)
    return (
        values_f
        * lax.rsqrt(jnp.mean(values_f * values_f, axis=-1, keepdims=True) + epsilon)
        * gain_row
    )


def attend_kernel(groups, query_ref, span_ref, bias_ref, cache_ref, out_ref, held, logits, sems):
    seqs, heads, _ = query_ref.shape
    length = cache_ref.shape[1]
    width = 256
    count = length // width
    copies = []
    for s in range(seqs):
        copy = pltpu.make_async_copy(cache_ref.at[s], held.at[s], sems.at[s])
        copy.start()
        copies.append(copy)
    table = (
        lax.broadcasted_iota(jnp.int32, (width, width), 0)
        >= lax.broadcasted_iota(jnp.int32, (width, width), 1)
    ).astype(F32)
    per_group = seqs // groups
    rows = per_group * heads
    for g in range(groups):
        first = g * per_group
        for s in range(first, first + per_group):
            copies[s].wait()
            logits[s * heads : (s + 1) * heads, :] = lax.dot_general(
                query_ref[s], held[s], (((1,), (1,)), ((), ())), preferred_element_type=F32
            )
        span = slice(first * heads, first * heads + rows)
        row = lax.broadcasted_iota(jnp.int32, (rows, 1), 0)
        limit = jnp.zeros((rows, 1), jnp.int32)
        for s in range(per_group):
            limit = jnp.where(row // heads == s, span_ref[first + s], limit)
        offset = jnp.zeros((rows, 1), F32)
        for h in range(heads):
            offset = jnp.where(row % heads == h, bias_ref[h], offset)
        carried = jnp.zeros((rows, 1), F32)
        for b in range(count - 1, -1, -1):
            cols = slice(b * width, (b + 1) * width)
            z = logits[span, cols] * HEAD_DIM ** (-0.5) + offset
            position = lax.broadcasted_iota(jnp.int32, (rows, width), 1) + b * width
            usable = position < limit
            soft = jnp.where(usable, jnp.maximum(z, 0.0) + jnp.log1p(jnp.exp(-jnp.abs(z))), 0.0)
            behind = jnp.dot(soft, table, precision=lax.Precision.HIGHEST, preferred_element_type=F32)
            weight = jnp.where(usable, jnp.exp(z - behind - carried), 0.0)
            carried = carried + jnp.sum(soft, axis=1, keepdims=True)
            logits[span, cols] = weight
        for s in range(first, first + per_group):
            out_ref[s] = jnp.dot(
                logits[s * heads : (s + 1) * heads, :].astype(BF16),
                held[s],
                preferred_element_type=F32,
            )


def attend(query_grid, lengths, bias, cache):
    seqs, heads, lanes = query_grid.shape
    length = cache.shape[1]
    smem = pl.BlockSpec(memory_space=pltpu.SMEM)
    vmem = pl.BlockSpec(memory_space=pltpu.VMEM)
    return pl.pallas_call(
        functools.partial(attend_kernel, 2),
        out_shape=jax.ShapeDtypeStruct((seqs, heads, lanes), F32),
        in_specs=[vmem, smem, smem, pl.BlockSpec(memory_space=pl.ANY)],
        out_specs=vmem,
        scratch_shapes=[
            pltpu.VMEM((seqs, length, lanes), BF16),
            pltpu.VMEM((seqs * heads, length), F32),
            pltpu.SemaphoreType.DMA((seqs,)),
        ],
        compiler_params=pltpu.CompilerParams(vmem_limit_bytes=60 * 2**20),
    )(query_grid, lengths, bias, cache)


def reduce_rounds(own, landing, flip, zmasks, ymasks, cols, send_sem, recv_sem, sent):
    def push(block, goal, slot):
        copy = pltpu.make_async_remote_copy(
            src_ref=own.at[block, :, cols],
            dst_ref=landing.at[slot, :, cols],
            send_sem=send_sem.at[len(sent)],
            recv_sem=recv_sem.at[slot],
            device_id={"ep": flip(goal)},
            device_id_type=MESH,
        )
        copy.start()
        sent.append(copy)
        arrivals[slot] = copy

    def fold(block, slots):
        total = own[block, :, cols].astype(F32)
        for slot in slots:
            arrivals[slot].wait_recv()
            total = total + landing[slot, :, cols].astype(F32)
        return total

    arrivals = {}
    for y in (*ymasks, 0):
        for z in (*zmasks, 0):
            push(z + y + 1, 1, z + y)
    yield None
    for z in (*zmasks, 0):
        for y in ymasks:
            own[z + y, :, cols] = fold(z + y, [z + y]).astype(BF16)
            push(z + y, y, z + y + 1)
    yield None
    for z in zmasks:
        own[z, :, cols] = fold(z, [z, *(z + y + 1 for y in ymasks)]).astype(BF16)
        push(z, z, z + 1)
    yield None
    yield fold(0, [0, *(y + 1 for y in ymasks), *(z + 1 for z in zmasks)])


def mix_kernel(
    ranks_ep,
    ranks_tp,
    partial_ref,
    tokens_ref,
    gain_ref,
    vector_ref,
    routes_ref,
    portions_ref,
    sgate_ref,
    sup_ref,
    sdown_hbm,
    gate_hbm,
    up_hbm,
    down_hbm,
    out_ref,
    attn_in,
    residual_ref,
    gathered,
    hidden_ref,
    terms,
    terms_in,
    shared,
    shared_in,
    last,
    last_in,
    gate_w,
    up_w,
    down_w,
    sdown_w,
    load_sem,
    tp_send,
    tp_recv,
    ag_send,
    ag_recv,
    rs_send,
    rs_recv,
    sh_send,
    sh_recv,
    out_send,
    out_recv,
):
    me = lax.axis_index("ep")
    my_tp = lax.axis_index("tp")
    row_count, width = tokens_ref.shape
    experts = gate_w.shape[0]
    table_width = gathered.shape[2] - width
    all_rows = ranks_ep * row_count
    chips = ranks_ep // 2
    across = 1 << (chips.bit_length() - 1) // 2
    zmasks = [m * 2 * across for m in range(chips // across - 1, 0, -1)]
    ymasks = [m * 2 for m in range(across - 1, 0, -1)]

    def flip(mask):
        index = me
        weight = 1
        while weight <= mask:
            if mask & weight:
                index = index + (1 - 2 * ((me // weight) % 2)) * weight
            weight = weight * 2
        return index

    loads = []
    for i, (source, target) in enumerate(
        ((gate_hbm, gate_w), (up_hbm, up_w), (down_hbm, down_w), (sdown_hbm, sdown_w))
    ):
        load = pltpu.make_async_copy(source, target, load_sem.at[i])
        load.start()
        loads.append(load)

    barrier = pltpu.get_barrier_semaphore()
    for mask in (*zmasks, *ymasks, 1):
        pl.semaphore_signal(barrier, inc=1, device_id={"ep": flip(mask)}, device_id_type=MESH)
    for step in range(1, ranks_tp):
        pl.semaphore_signal(
            barrier, inc=1, device_id={"tp": lax.rem(my_tp + step, ranks_tp)}, device_id_type=MESH
        )
    pl.semaphore_wait(barrier, len(zmasks) + len(ymasks) + ranks_tp)

    swaps = []
    for step in range(1, ranks_tp):
        swap = pltpu.make_async_remote_copy(
            src_ref=partial_ref,
            dst_ref=attn_in.at[step - 1],
            send_sem=tp_send.at[step - 1],
            recv_sem=tp_recv.at[step - 1],
            device_id={"tp": lax.rem(my_tp + step, ranks_tp)},
            device_id_type=MESH,
        )
        swap.start()
        swaps.append(swap)

    lane = lax.broadcasted_iota(jnp.int32, (row_count, table_width), 1)
    stride = table_width // 2
    table = jnp.zeros((row_count, table_width), F32)
    for k in range(routes_ref.shape[1]):
        named = routes_ref[:, k : k + 1]
        portion = portions_ref[:, k : k + 1]
        high = portion.astype(BF16).astype(F32)
        table = jnp.where(lane == named, high, table)
        table = jnp.where(lane == named + stride, portion - high, table)
    gathered[0, :, width:] = table.astype(BF16)

    residual = partial_ref[...].astype(F32)
    for step in range(1, ranks_tp):
        swaps[step - 1].wait()
        residual = residual + attn_in[step - 1].astype(F32)
    residual = residual + tokens_ref[...].astype(F32)
    residual_ref[...] = residual
    normed = (
        residual
        * lax.rsqrt(jnp.mean(residual * residual, axis=-1, keepdims=True) + epsilon)
        * gain_ref[...]
    ).astype(BF16)
    gathered[0, :, :width] = normed

    sent = []
    arrivals = {}

    def share(block, goal):
        slot = block ^ goal
        copy = pltpu.make_async_remote_copy(
            src_ref=gathered.at[block],
            dst_ref=gathered.at[slot],
            send_sem=ag_send.at[len(sent)],
            recv_sem=ag_recv.at[slot],
            device_id={"ep": flip(goal)},
            device_id_type=MESH,
        )
        copy.start()
        sent.append(copy)
        arrivals[slot] = copy

    for mask in (*zmasks, *ymasks, 1):
        share(0, mask)
    mix_gate = jax.nn.sigmoid(
        jnp.sum(normed.astype(F32) * vector_ref[...].astype(F32), axis=1, keepdims=True)
    )
    for y in ymasks:
        arrivals[y].wait_recv()
        share(y, 1)
    for z in zmasks:
        arrivals[z].wait_recv()
        for y in ymasks:
            share(z, y)
        share(z, 1)
    for z in zmasks:
        for y in ymasks:
            arrivals[z + y].wait_recv()
            share(z + y, 1)
    for z in (*zmasks, 0):
        for y in (*ymasks, 0):
            arrivals[z + y + 1].wait_recv()

    shared_cols = sgate_ref.shape[1]
    depth = sgate_ref.shape[0]
    feature_at = pl.ds(pl.multiple_of(me * (width // ranks_ep) // depth * depth, depth), depth)
    features = gathered[:, :, feature_at].reshape(all_rows, depth)
    for i, part in enumerate((sgate_ref, sup_ref)):
        shared[:, :, i * shared_cols : (i + 1) * shared_cols] = (
            jnp.dot(features, part[...], preferred_element_type=F32)
            .astype(BF16)
            .reshape(ranks_ep, row_count, shared_cols)
        )
    shared_sent = []
    shared_rounds = reduce_rounds(
        shared,
        shared_in,
        flip,
        zmasks,
        ymasks,
        slice(None),
        sh_send,
        sh_recv,
        shared_sent,
    )
    next(shared_rounds)
    rows = gathered[:, :, :width].reshape(all_rows, width)
    route_cols = gathered[:, :, width:].reshape(all_rows, table_width).astype(F32)
    lanes = lax.broadcasted_iota(jnp.int32, route_cols.shape, 1)
    loads[0].wait()
    loads[1].wait()
    scales = []
    for j in range(experts):
        wanted = me * experts + j
        chosen = jnp.where((lanes == wanted) | (lanes == wanted + stride), route_cols, 0.0)
        scales.append(jnp.sum(chosen, axis=1, keepdims=True))
        gate_val = jnp.dot(rows, gate_w[j], preferred_element_type=F32)
        up_val = jnp.dot(rows, up_w[j], preferred_element_type=F32)
        hidden_ref[j] = (gate_val * jax.nn.sigmoid(gate_val) * up_val).astype(BF16)
    next(shared_rounds)
    loads[2].wait()
    loads[3].wait()
    half = width // 2
    term_sent = []
    rounds = []
    for s in range(2):
        cols = slice(s * half, (s + 1) * half)
        term = jnp.zeros((all_rows, half), F32)
        for j in range(experts):
            term = term + scales[j] * jnp.dot(
                hidden_ref[j], down_w[j, :, cols], preferred_element_type=F32
            )
        terms[:, :, cols] = term.astype(BF16).reshape(ranks_ep, row_count, half)
        term_sent.append([])
        rounds.append(
            reduce_rounds(
                terms,
                terms_in,
                flip,
                zmasks,
                ymasks,
                cols,
                rs_send.at[s],
                rs_recv.at[s],
                term_sent[s],
            )
        )
        next(rounds[s])
        if s == 0:
            next(shared_rounds)
    for turn in range(2):
        for s in range(2):
            next(rounds[s])
    total = next(shared_rounds)
    gate_sum = total[:, :shared_cols]
    up_sum = total[:, shared_cols:]
    shared_hidden = (gate_sum * jax.nn.sigmoid(gate_sum) * up_sum).astype(BF16)
    shared_term = mix_gate * jnp.dot(shared_hidden, sdown_w[...], preferred_element_type=F32)
    for s in range(2):
        cols = slice(s * half, (s + 1) * half)
        last[:, cols] = (next(rounds[s]) + shared_term[:, cols]).astype(BF16)
    quarter = width // ranks_tp

    def quarter_of(index):
        return pl.ds(pl.multiple_of(index * quarter, quarter), quarter)

    ends = []
    for step in range(1, ranks_tp):
        goal = lax.rem(my_tp + step, ranks_tp)
        end = pltpu.make_async_remote_copy(
            src_ref=last.at[:, quarter_of(goal)],
            dst_ref=last_in.at[step - 1],
            send_sem=out_send.at[step - 1],
            recv_sem=out_recv.at[step - 1],
            device_id={"tp": goal},
            device_id_type=MESH,
        )
        end.start()
        ends.append(end)
    for copy in (*sent, *shared_sent, *term_sent[0], *term_sent[1]):
        copy.wait_send()
    result = residual_ref[:, quarter_of(my_tp)] + last[:, quarter_of(my_tp)].astype(F32)
    for step in range(1, ranks_tp):
        ends[step - 1].wait()
        result = result + last_in[step - 1].astype(F32)
    out_ref[...] = result.astype(BF16)


def mix(
    ranks_ep,
    ranks_tp,
    attn_term,
    tokens,
    ffn_gain,
    gate_vector,
    routes,
    route_weights,
    shared_gate,
    shared_up,
    shared_down,
    expert_gate,
    expert_up,
    expert_down,
):
    row_count, width = tokens.shape
    grid = (ranks_ep, row_count)
    experts, _, hidden = expert_gate.shape
    shared_cols = shared_gate.shape[1]
    quarter = width // ranks_tp
    table_width = -(-2 * ranks_ep * experts // LANES) * LANES
    swaps = max(ranks_tp - 1, 1)
    vmem = pl.BlockSpec(memory_space=pltpu.VMEM)
    anywhere = pl.BlockSpec(memory_space=pl.ANY)
    dma = pltpu.SemaphoreType.DMA
    return pl.pallas_call(
        functools.partial(mix_kernel, ranks_ep, ranks_tp),
        out_shape=jax.ShapeDtypeStruct((row_count, quarter), BF16),
        in_specs=[vmem] * 8 + [anywhere] * 4,
        out_specs=vmem,
        scratch_shapes=[
            pltpu.VMEM((swaps, row_count, width), BF16),
            pltpu.VMEM((row_count, width), F32),
            pltpu.VMEM((*grid, width + table_width), BF16),
            pltpu.VMEM((experts, ranks_ep * row_count, hidden), BF16),
            pltpu.VMEM((*grid, width), BF16),
            pltpu.VMEM((*grid, width), BF16),
            pltpu.VMEM((*grid, 2 * shared_cols), BF16),
            pltpu.VMEM((*grid, 2 * shared_cols), BF16),
            pltpu.VMEM((row_count, width), BF16),
            pltpu.VMEM((swaps, row_count, quarter), BF16),
            pltpu.VMEM(expert_gate.shape, BF16),
            pltpu.VMEM(expert_up.shape, BF16),
            pltpu.VMEM(expert_down.shape, BF16),
            pltpu.VMEM(shared_down.shape, BF16),
            dma((4,)),
            dma((swaps,)),
            dma((swaps,)),
            dma((ranks_ep,)),
            dma((ranks_ep,)),
            dma((2, ranks_ep)),
            dma((2, ranks_ep)),
            dma((ranks_ep,)),
            dma((ranks_ep,)),
            dma((swaps,)),
            dma((swaps,)),
        ],
        compiler_params=pltpu.CompilerParams(
            collective_id=0, has_side_effects=True, vmem_limit_bytes=60 * 2**20
        ),
    )(
        attn_term,
        tokens,
        ffn_gain.reshape(1, width),
        gate_vector.reshape(1, width),
        routes,
        route_weights,
        shared_gate,
        shared_up,
        shared_down,
        expert_gate,
        expert_up,
        expert_down,
    )


def shards(
    ranks_ep,
    ranks_tp,
    tokens,
    lengths,
    cache,
    attn_gain,
    query_weight,
    key_weight,
    value_weight,
    stick_bias,
    out_weight,
    ffn_gain,
    routes,
    route_weights,
    expert_gate,
    expert_up,
    expert_down,
    shared_gate,
    shared_up,
    shared_down,
    gate_vector,
):
    row_count = tokens.shape[0]
    normed = rms_scale(tokens, attn_gain).astype(BF16)
    queries = jnp.dot(normed, query_weight, preferred_element_type=F32).astype(BF16)
    key_rows = jnp.dot(normed, key_weight, preferred_element_type=F32).astype(BF16)
    value_rows = jnp.dot(normed, value_weight, preferred_element_type=F32).astype(BF16)
    heads = key_weight.shape[1] // HEAD_DIM
    new_kv = jnp.stack(
        [
            key_rows.reshape(row_count, heads, HEAD_DIM),
            value_rows.reshape(row_count, heads, HEAD_DIM),
        ],
        axis=2,
    ).reshape(row_count, heads * 2 * HEAD_DIM)
    group = queries.shape[1] // HEAD_DIM // heads
    same = jnp.eye(heads, dtype=jnp.bool_)
    spread = jnp.where(
        same[None, :, None, :, None],
        queries.reshape(row_count, heads, group, 1, HEAD_DIM),
        jnp.zeros((), BF16),
    )
    spread = jnp.pad(spread, ((0, 0),) * 4 + ((0, HEAD_DIM),))
    query_grid = spread.reshape(row_count, heads * group, heads * 2 * HEAD_DIM)
    mixed = attend(query_grid, lengths, stick_bias, cache)
    mixed = mixed.reshape(row_count, heads, group, heads, 2 * HEAD_DIM)[..., HEAD_DIM:]
    heads_out = jnp.sum(jnp.where(same[None, :, None, :, None], mixed, 0.0), axis=3).astype(BF16)
    attn_term = jnp.dot(
        heads_out.reshape(row_count, -1), out_weight, preferred_element_type=F32
    ).astype(BF16)
    depth = shared_gate.shape[0]
    if depth % LANES:
        slot = lax.axis_index("ep") * depth % LANES
        wide = jnp.zeros((LANES, shared_gate.shape[1]), BF16)
        shared_gate = lax.dynamic_update_slice_in_dim(wide, shared_gate, slot, 0)
        shared_up = lax.dynamic_update_slice_in_dim(wide, shared_up, slot, 0)
    layer_out = mix(
        ranks_ep,
        ranks_tp,
        attn_term,
        tokens,
        ffn_gain,
        gate_vector,
        routes,
        route_weights,
        shared_gate,
        shared_up,
        shared_down,
        expert_gate,
        expert_up,
        expert_down,
    )
    return (layer_out, new_kv)


def solution(mesh):
    placed = (
        P("ep", None),
        P("ep"),
        P("ep", None, "tp"),
        P(),
        P(None, "tp"),
        P(None, "tp"),
        P(None, "tp"),
        P("tp"),
        P("tp", None),
        P(),
        P("ep", None),
        P("ep", None),
        P("ep", None, "tp"),
        P("ep", None, "tp"),
        P("ep", "tp", None),
        P("ep", "tp"),
        P("ep", "tp"),
        P("tp", None),
        P(),
    )
    return jax.shard_map(
        functools.partial(shards, mesh.shape["ep"], mesh.shape["tp"]),
        mesh=mesh,
        in_specs=placed,
        out_specs=(P("ep", "tp"), P("ep", "tp")),
        check_vma=False,
    )
```

```python
import functools

import jax
import jax.numpy as jnp
from jax import lax
from jax.experimental import pallas as pl
from jax.experimental.pallas import tpu as pltpu
from jax.sharding import PartitionSpec as P

HEAD_DIM = 64
LANES = 128
epsilon = 1e-06
MESH = pl.DeviceIdType.MESH
F32 = jnp.float32
BF16 = jnp.bfloat16


def rms_scale(rows_in, gain_row):
    values_f = rows_in.astype(F32)
    return (
        values_f
        * lax.rsqrt(jnp.mean(values_f * values_f, axis=-1, keepdims=True) + epsilon)
        * gain_row
    )


def attend_kernel(groups, query_ref, span_ref, bias_ref, cache_ref, out_ref, held, logits, spread, sems):
    seqs, heads, _ = spread.shape
    tiles = spread.shape[2] // LANES
    group = heads // tiles
    first_half = lax.broadcasted_iota(jnp.int32, (seqs, LANES), 1) < HEAD_DIM
    length = cache_ref.shape[1]
    width = 256
    count = length // width
    copies = []
    for s in range(seqs):
        copy = pltpu.make_async_copy(cache_ref.at[s], held.at[s], sems.at[s])
        copy.start()
        copies.append(copy)
    spread[...] = jnp.zeros_like(spread)
    for h in range(heads):
        pair = query_ref[:, h // 2 * LANES : (h // 2 + 1) * LANES].astype(F32)
        if h % 2:
            pair = pltpu.roll(pair, HEAD_DIM, 1)
        tile = h // group * LANES
        spread[:, h, tile : tile + LANES] = jnp.where(first_half, pair, 0.0)
    table = (
        lax.broadcasted_iota(jnp.int32, (width, width), 0)
        >= lax.broadcasted_iota(jnp.int32, (width, width), 1)
    ).astype(F32)
    per_group = seqs // groups
    rows = per_group * heads
    for g in range(groups):
        first = g * per_group
        for s in range(first, first + per_group):
            copies[s].wait()
            logits[s * heads : (s + 1) * heads, :] = lax.dot_general(
                spread[s].astype(BF16), held[s], (((1,), (1,)), ((), ())), preferred_element_type=F32
            )
        span = slice(first * heads, first * heads + rows)
        row = lax.broadcasted_iota(jnp.int32, (rows, 1), 0)
        limit = jnp.zeros((rows, 1), jnp.int32)
        for s in range(per_group):
            limit = jnp.where(row // heads == s, span_ref[first + s], limit)
        offset = jnp.zeros((rows, 1), F32)
        for h in range(heads):
            offset = jnp.where(row % heads == h, bias_ref[h], offset)
        carried = jnp.zeros((rows, 1), F32)
        for b in range(count - 1, -1, -1):
            cols = slice(b * width, (b + 1) * width)
            z = logits[span, cols] * HEAD_DIM ** (-0.5) + offset
            position = lax.broadcasted_iota(jnp.int32, (rows, width), 1) + b * width
            usable = position < limit
            soft = jnp.where(usable, jnp.maximum(z, 0.0) + jnp.log1p(jnp.exp(-jnp.abs(z))), 0.0)
            behind = jnp.dot(soft, table, precision=lax.Precision.HIGHEST, preferred_element_type=F32)
            weight = jnp.where(usable, jnp.exp(z - behind - carried), 0.0)
            carried = carried + jnp.sum(soft, axis=1, keepdims=True)
            logits[span, cols] = weight
        for s in range(first, first + per_group):
            spread[s] = jnp.dot(
                logits[s * heads : (s + 1) * heads, :].astype(BF16),
                held[s],
                preferred_element_type=F32,
            )
    for i in range(heads // 2):
        pair = []
        for h in (2 * i, 2 * i + 1):
            tile = h // group * LANES
            pair.append(spread[:, h, tile : tile + LANES])
        both = jnp.where(first_half, pltpu.roll(pair[0], HEAD_DIM, 1), pair[1])
        out_ref[:, i * LANES : (i + 1) * LANES] = both.astype(BF16)


def attend(queries, lengths, bias, cache):
    seqs = queries.shape[0]
    heads = queries.shape[1] // HEAD_DIM
    length, lanes = cache.shape[1:]
    smem = pl.BlockSpec(memory_space=pltpu.SMEM)
    vmem = pl.BlockSpec(memory_space=pltpu.VMEM)
    return pl.pallas_call(
        functools.partial(attend_kernel, 2),
        out_shape=jax.ShapeDtypeStruct(queries.shape, BF16),
        in_specs=[vmem, smem, smem, pl.BlockSpec(memory_space=pl.ANY)],
        out_specs=vmem,
        scratch_shapes=[
            pltpu.VMEM((seqs, length, lanes), BF16),
            pltpu.VMEM((seqs * heads, length), F32),
            pltpu.VMEM((seqs, heads, lanes), F32),
            pltpu.SemaphoreType.DMA((seqs,)),
        ],
        compiler_params=pltpu.CompilerParams(vmem_limit_bytes=60 * 2**20),
    )(queries, lengths, bias, cache)


def reduce_rounds(own, landing, flip, zmasks, ymasks, cols, send_sem, recv_sem, sent):
    def push(block, goal, slot):
        copy = pltpu.make_async_remote_copy(
            src_ref=own.at[block, :, cols],
            dst_ref=landing.at[slot, :, cols],
            send_sem=send_sem.at[len(sent)],
            recv_sem=recv_sem.at[slot],
            device_id={"ep": flip(goal)},
            device_id_type=MESH,
        )
        copy.start()
        sent.append(copy)
        arrivals[slot] = copy

    def fold(block, slots):
        total = own[block, :, cols].astype(F32)
        for slot in slots:
            arrivals[slot].wait_recv()
            total = total + landing[slot, :, cols].astype(F32)
        return total

    arrivals = {}
    for y in (*ymasks, 0):
        for z in (*zmasks, 0):
            push(z + y + 1, 1, z + y)
    yield None
    for z in (*zmasks, 0):
        for y in ymasks:
            own[z + y, :, cols] = fold(z + y, [z + y]).astype(BF16)
            push(z + y, y, z + y + 1)
    yield None
    for z in zmasks:
        own[z, :, cols] = fold(z, [z, *(z + y + 1 for y in ymasks)]).astype(BF16)
        push(z, z, z + 1)
    yield None
    yield fold(0, [0, *(y + 1 for y in ymasks), *(z + 1 for z in zmasks)])


def mix_kernel(
    ranks_ep,
    ranks_tp,
    partial_ref,
    tokens_ref,
    gain_ref,
    vector_ref,
    routes_ref,
    portions_ref,
    sgate_ref,
    sup_ref,
    sdown_hbm,
    gate_hbm,
    up_hbm,
    down_hbm,
    out_ref,
    attn_in,
    residual_ref,
    gathered,
    hidden_ref,
    terms,
    terms_in,
    shared,
    shared_in,
    last,
    last_in,
    gate_w,
    up_w,
    down_w,
    sdown_w,
    load_sem,
    tp_send,
    tp_recv,
    ag_send,
    ag_recv,
    rs_send,
    rs_recv,
    sh_send,
    sh_recv,
    out_send,
    out_recv,
):
    me = lax.axis_index("ep")
    my_tp = lax.axis_index("tp")
    row_count, width = tokens_ref.shape
    experts = gate_w.shape[0]
    table_width = gathered.shape[2] - width
    all_rows = ranks_ep * row_count
    chips = ranks_ep // 2
    across = 1 << (chips.bit_length() - 1) // 2
    zmasks = [m * 2 * across for m in range(chips // across - 1, 0, -1)]
    ymasks = [m * 2 for m in range(across - 1, 0, -1)]

    def flip(mask):
        index = me
        weight = 1
        while weight <= mask:
            if mask & weight:
                index = index + (1 - 2 * ((me // weight) % 2)) * weight
            weight = weight * 2
        return index

    loads = []
    for i, (source, target) in enumerate(
        ((gate_hbm, gate_w), (up_hbm, up_w), (down_hbm, down_w), (sdown_hbm, sdown_w))
    ):
        load = pltpu.make_async_copy(source, target, load_sem.at[i])
        load.start()
        loads.append(load)

    barrier = pltpu.get_barrier_semaphore()
    for mask in (*zmasks, *ymasks, 1):
        pl.semaphore_signal(barrier, inc=1, device_id={"ep": flip(mask)}, device_id_type=MESH)
    for step in range(1, ranks_tp):
        pl.semaphore_signal(
            barrier, inc=1, device_id={"tp": lax.rem(my_tp + step, ranks_tp)}, device_id_type=MESH
        )
    pl.semaphore_wait(barrier, len(zmasks) + len(ymasks) + ranks_tp)

    swaps = []
    for step in range(1, ranks_tp):
        swap = pltpu.make_async_remote_copy(
            src_ref=partial_ref,
            dst_ref=attn_in.at[step - 1],
            send_sem=tp_send.at[step - 1],
            recv_sem=tp_recv.at[step - 1],
            device_id={"tp": lax.rem(my_tp + step, ranks_tp)},
            device_id_type=MESH,
        )
        swap.start()
        swaps.append(swap)

    lane = lax.broadcasted_iota(jnp.int32, (row_count, table_width), 1)
    stride = table_width // 2
    table = jnp.zeros((row_count, table_width), F32)
    route_ids = jnp.transpose(routes_ref[...])
    portions = jnp.transpose(portions_ref[...])
    for k in range(routes_ref.shape[0]):
        named = route_ids[:, k : k + 1]
        portion = portions[:, k : k + 1]
        high = portion.astype(BF16).astype(F32)
        table = jnp.where(lane == named, high, table)
        table = jnp.where(lane == named + stride, portion - high, table)
    gathered[0, :, width:] = table.astype(BF16)

    residual = partial_ref[...].astype(F32)
    for step in range(1, ranks_tp):
        swaps[step - 1].wait()
        residual = residual + attn_in[step - 1].astype(F32)
    residual = residual + tokens_ref[...].astype(F32)
    residual_ref[...] = residual
    normed = (
        residual
        * lax.rsqrt(jnp.mean(residual * residual, axis=-1, keepdims=True) + epsilon)
        * gain_ref[...]
    ).astype(BF16)
    gathered[0, :, :width] = normed

    sent = []
    arrivals = {}

    def share(block, goal):
        slot = block ^ goal
        copy = pltpu.make_async_remote_copy(
            src_ref=gathered.at[block],
            dst_ref=gathered.at[slot],
            send_sem=ag_send.at[len(sent)],
            recv_sem=ag_recv.at[slot],
            device_id={"ep": flip(goal)},
            device_id_type=MESH,
        )
        copy.start()
        sent.append(copy)
        arrivals[slot] = copy

    for mask in (*zmasks, *ymasks, 1):
        share(0, mask)
    mix_gate = jax.nn.sigmoid(
        jnp.sum(normed.astype(F32) * vector_ref[...].astype(F32).reshape(1, width), axis=1, keepdims=True)
    )
    for y in ymasks:
        arrivals[y].wait_recv()
        share(y, 1)
    for z in zmasks:
        arrivals[z].wait_recv()
        for y in ymasks:
            share(z, y)
        share(z, 1)
    for z in zmasks:
        for y in ymasks:
            arrivals[z + y].wait_recv()
            share(z + y, 1)
    for z in (*zmasks, 0):
        for y in (*ymasks, 0):
            arrivals[z + y + 1].wait_recv()

    shared_cols = sgate_ref.shape[1]
    depth = sgate_ref.shape[0]
    feature_at = pl.ds(pl.multiple_of(me * (width // ranks_ep) // depth * depth, depth), depth)
    features = gathered[:, :, feature_at].reshape(all_rows, depth)
    for i, part in enumerate((sgate_ref, sup_ref)):
        shared[:, :, i * shared_cols : (i + 1) * shared_cols] = (
            jnp.dot(features, part[...], preferred_element_type=F32)
            .astype(BF16)
            .reshape(ranks_ep, row_count, shared_cols)
        )
    shared_sent = []
    shared_rounds = reduce_rounds(
        shared,
        shared_in,
        flip,
        zmasks,
        ymasks,
        slice(None),
        sh_send,
        sh_recv,
        shared_sent,
    )
    next(shared_rounds)
    rows = gathered[:, :, :width].reshape(all_rows, width)
    route_cols = gathered[:, :, width:].reshape(all_rows, table_width).astype(F32)
    lanes = lax.broadcasted_iota(jnp.int32, route_cols.shape, 1)
    loads[0].wait()
    loads[1].wait()
    scales = []
    for j in range(experts):
        wanted = me * experts + j
        chosen = jnp.where((lanes == wanted) | (lanes == wanted + stride), route_cols, 0.0)
        scales.append(jnp.sum(chosen, axis=1, keepdims=True))
        gate_val = jnp.dot(rows, gate_w[j], preferred_element_type=F32)
        up_val = jnp.dot(rows, up_w[j], preferred_element_type=F32)
        hidden_ref[j] = (gate_val * jax.nn.sigmoid(gate_val) * up_val).astype(BF16)
    next(shared_rounds)
    loads[2].wait()
    loads[3].wait()
    half = width // 2
    term_sent = []
    rounds = []
    for s in range(2):
        cols = slice(s * half, (s + 1) * half)
        term = jnp.zeros((all_rows, half), F32)
        for j in range(experts):
            term = term + scales[j] * jnp.dot(
                hidden_ref[j], down_w[j, :, cols], preferred_element_type=F32
            )
        terms[:, :, cols] = term.astype(BF16).reshape(ranks_ep, row_count, half)
        term_sent.append([])
        rounds.append(
            reduce_rounds(
                terms,
                terms_in,
                flip,
                zmasks,
                ymasks,
                cols,
                rs_send.at[s],
                rs_recv.at[s],
                term_sent[s],
            )
        )
        next(rounds[s])
        if s == 0:
            next(shared_rounds)
    for turn in range(2):
        for s in range(2):
            next(rounds[s])
    total = next(shared_rounds)
    gate_sum = total[:, :shared_cols]
    up_sum = total[:, shared_cols:]
    shared_hidden = (gate_sum * jax.nn.sigmoid(gate_sum) * up_sum).astype(BF16)
    shared_term = mix_gate * jnp.dot(shared_hidden, sdown_w[...], preferred_element_type=F32)
    for s in range(2):
        cols = slice(s * half, (s + 1) * half)
        last[:, cols] = (next(rounds[s]) + shared_term[:, cols]).astype(BF16)
    quarter = width // ranks_tp

    def quarter_of(index):
        return pl.ds(pl.multiple_of(index * quarter, quarter), quarter)

    ends = []
    for step in range(1, ranks_tp):
        goal = lax.rem(my_tp + step, ranks_tp)
        end = pltpu.make_async_remote_copy(
            src_ref=last.at[:, quarter_of(goal)],
            dst_ref=last_in.at[step - 1],
            send_sem=out_send.at[step - 1],
            recv_sem=out_recv.at[step - 1],
            device_id={"tp": goal},
            device_id_type=MESH,
        )
        end.start()
        ends.append(end)
    for copy in (*sent, *shared_sent, *term_sent[0], *term_sent[1]):
        copy.wait_send()
    result = residual_ref[:, quarter_of(my_tp)] + last[:, quarter_of(my_tp)].astype(F32)
    for step in range(1, ranks_tp):
        ends[step - 1].wait()
        result = result + last_in[step - 1].astype(F32)
    out_ref[...] = result


def mix(
    ranks_ep,
    ranks_tp,
    attn_term,
    tokens,
    ffn_gain,
    gate_vector,
    routes,
    route_weights,
    shared_gate,
    shared_up,
    shared_down,
    expert_gate,
    expert_up,
    expert_down,
):
    row_count, width = tokens.shape
    grid = (ranks_ep, row_count)
    experts, _, hidden = expert_gate.shape
    shared_cols = shared_gate.shape[1]
    quarter = width // ranks_tp
    table_width = -(-2 * ranks_ep * experts // LANES) * LANES
    swaps = max(ranks_tp - 1, 1)
    vmem = pl.BlockSpec(memory_space=pltpu.VMEM)
    anywhere = pl.BlockSpec(memory_space=pl.ANY)
    dma = pltpu.SemaphoreType.DMA
    return pl.pallas_call(
        functools.partial(mix_kernel, ranks_ep, ranks_tp),
        out_shape=jax.ShapeDtypeStruct((row_count, quarter), F32),
        in_specs=[vmem] * 8 + [anywhere] * 4,
        out_specs=vmem,
        scratch_shapes=[
            pltpu.VMEM((swaps, row_count, width), BF16),
            pltpu.VMEM((row_count, width), F32),
            pltpu.VMEM((*grid, width + table_width), BF16),
            pltpu.VMEM((experts, ranks_ep * row_count, hidden), BF16),
            pltpu.VMEM((*grid, width), BF16),
            pltpu.VMEM((*grid, width), BF16),
            pltpu.VMEM((*grid, 2 * shared_cols), BF16),
            pltpu.VMEM((*grid, 2 * shared_cols), BF16),
            pltpu.VMEM((row_count, width), BF16),
            pltpu.VMEM((swaps, row_count, quarter), BF16),
            pltpu.VMEM(expert_gate.shape, BF16),
            pltpu.VMEM(expert_up.shape, BF16),
            pltpu.VMEM(expert_down.shape, BF16),
            pltpu.VMEM(shared_down.shape, BF16),
            dma((4,)),
            dma((swaps,)),
            dma((swaps,)),
            dma((ranks_ep,)),
            dma((ranks_ep,)),
            dma((2, ranks_ep)),
            dma((2, ranks_ep)),
            dma((ranks_ep,)),
            dma((ranks_ep,)),
            dma((swaps,)),
            dma((swaps,)),
        ],
        compiler_params=pltpu.CompilerParams(
            collective_id=0, has_side_effects=True, vmem_limit_bytes=60 * 2**20
        ),
    )(
        attn_term,
        tokens,
        ffn_gain.reshape(1, width),
        gate_vector,
        routes.T,
        route_weights.T,
        shared_gate,
        shared_up,
        shared_down,
        expert_gate,
        expert_up,
        expert_down,
    )


def shards(
    ranks_ep,
    ranks_tp,
    tokens,
    lengths,
    cache,
    attn_gain,
    query_weight,
    key_weight,
    value_weight,
    stick_bias,
    out_weight,
    ffn_gain,
    routes,
    route_weights,
    expert_gate,
    expert_up,
    expert_down,
    shared_gate,
    shared_up,
    shared_down,
    gate_vector,
):
    row_count = tokens.shape[0]
    normed = rms_scale(tokens, attn_gain).astype(BF16)
    queries = jnp.dot(normed, query_weight, preferred_element_type=F32).astype(BF16)
    key_rows = jnp.dot(normed, key_weight, preferred_element_type=F32).astype(BF16)
    value_rows = jnp.dot(normed, value_weight, preferred_element_type=F32).astype(BF16)
    heads = key_weight.shape[1] // HEAD_DIM
    new_kv = jnp.stack(
        [
            key_rows.reshape(row_count, heads, HEAD_DIM),
            value_rows.reshape(row_count, heads, HEAD_DIM),
        ],
        axis=2,
    ).reshape(row_count, heads * 2 * HEAD_DIM)
    heads_out = attend(queries, lengths, stick_bias, cache)
    attn_term = jnp.dot(
        heads_out, out_weight, preferred_element_type=F32
    ).astype(BF16)
    depth = shared_gate.shape[0]
    if depth % LANES:
        slot = lax.axis_index("ep") * depth % LANES
        wide = jnp.zeros((LANES, shared_gate.shape[1]), BF16)
        shared_gate = lax.dynamic_update_slice_in_dim(wide, shared_gate, slot, 0)
        shared_up = lax.dynamic_update_slice_in_dim(wide, shared_up, slot, 0)
    layer_out = mix(
        ranks_ep,
        ranks_tp,
        attn_term,
        tokens,
        ffn_gain,
        gate_vector,
        routes,
        route_weights,
        shared_gate,
        shared_up,
        shared_down,
        expert_gate,
        expert_up,
        expert_down,
    )
    return (layer_out.astype(BF16), new_kv)


def solution(mesh):
    placed = (
        P("ep", None),
        P("ep"),
        P("ep", None, "tp"),
        P(),
        P(None, "tp"),
        P(None, "tp"),
        P(None, "tp"),
        P("tp"),
        P("tp", None),
        P(),
        P("ep", None),
        P("ep", None),
        P("ep", None, "tp"),
        P("ep", None, "tp"),
        P("ep", "tp", None),
        P("ep", "tp"),
        P("ep", "tp"),
        P("tp", None),
        P(),
    )
    return jax.shard_map(
        functools.partial(shards, mesh.shape["ep"], mesh.shape["tp"]),
        mesh=mesh,
        in_specs=placed,
        out_specs=(P("ep", "tp"), P("ep", "tp")),
        check_vma=False,
    )
```
